32 devices in a mesh: sp: 4 (over z), dp: 8 (over y, x, core).
Axes of the slice: x: 2, y: 2, z: 4, core: 2. Of those that a mesh axis runs over, the one named last changes fastest.
Arguments:
- inputs: bfloat16 [8, 512, 2048], P('dp', 'sp'), may hold values from -6 to 6
- queries: bfloat16 [8, 512, 1024], P('dp', 'sp'), may hold values from -6 to 6
- keys: bfloat16 [8, 512, 1024], P('dp', 'sp'), may hold values from -1.5 to 1.5
- values: bfloat16 [8, 512, 1024], P('dp', 'sp'), may hold values from -6 to 6
- log_decay: bfloat16 [8, 512, 1024], P('dp', 'sp'), may hold values from -0.1 to 0, as said below
- cotangent: bfloat16 [8, 512, 1024], P('dp', 'sp'), may hold values from -0.59765625 to 0.59765625
- value_weight: bfloat16 [2048, 1024], P('dp'), may hold values from -0.125 to 0.125
Outputs:
- grad_queries: bfloat16 [8, 512, 1024], P('dp', 'sp')
- grad_keys: bfloat16 [8, 512, 1024], P('dp', 'sp')
- grad_decay: bfloat16 [8, 512, 1024], P('dp', 'sp')
- grad_inputs: bfloat16 [8, 512, 2048], P('dp', 'sp')
- grad_weight: float32 [2048, 1024], P('dp')
The draws below stay inside these ranges and needn't reach their ends.
Inputs may be any that keep to these rules, and one draw needn't show every extreme that they name: `log_decay`: the log decays are negative; per key channel and sequence they differ between positions.
All inputs are finite; a program needn't handle non-finite values.
Results may differ from the reference program's by a relative error of at most 0.015.
Values may be sent and summed in bfloat16 or wider, within the bound.
No kernel may reach another device: no remote copies, remote signals or barrier semaphores. Data moves between devices by JAX's collectives and lax.ppermute only.
A program may use at most 128 MiB of HBM per device.

```python
import math
import jax
import jax.numpy as jnp
from jax import lax

D = 2048
HEADS = 16
HEAD_DIM = 64
BLOCK = 128
HALF = 32
GROUPS = 32
WIDTH = 1024
SEQ = 512
SEQS = 8


def draw_log_decay(key, part):
    keys_list = jax.random.split(key, 5)
    share = 0.5
    slow_pick = jax.random.uniform(keys_list[0], (SEQS, 1, WIDTH), jnp.float32) < share
    fast_rate = jax.random.uniform(keys_list[1], (SEQS, 1, WIDTH), jnp.float32, 1.0 / 50.0, 1.0 / 30.0)
    slow_rate = jax.random.uniform(keys_list[2], (SEQS, 1, WIDTH), jnp.float32, 0.2, 0.5) / SEQ
    base_rate = jnp.where(slow_pick, slow_rate, fast_rate)
    block_count = SEQ // BLOCK
    block_factor = jnp.exp(jax.random.uniform(keys_list[3], (SEQS, block_count, 1, WIDTH), jnp.float32, -math.log(2.0), math.log(2.0)))
    block_factor = jnp.broadcast_to(block_factor, (SEQS, block_count, BLOCK, WIDTH)).reshape(SEQS, SEQ, WIDTH)
    token_factor = jnp.exp(jax.random.uniform(keys_list[4], (SEQS, SEQ, WIDTH), jnp.float32, math.log(0.7), math.log(1.4)))
    return (-(base_rate * block_factor * token_factor)).astype(jnp.bfloat16)


def levels(stream_key, extent, cuts, low, high):
    gain = 1.0
    for axis_at, parts in cuts:
        steps = jax.random.uniform(jax.random.fold_in(jax.random.fold_in(stream_key, 6), axis_at), (parts,), jnp.float32, low / len(cuts), high / len(cuts))
        gain = gain * jnp.repeat(jnp.exp(steps), extent[axis_at] // parts).reshape((-1,) + (1,) * (len(extent) - 1 - axis_at))
    return gain


def scatter_about(rng, shape, scale, limit, cuts=(), dtype=jnp.bfloat16):
    result = jax.random.normal(rng, shape, jnp.float32) * scale
    if len(cuts) > 0:
        result = levels(rng, shape, cuts, -0.22, 0.18) * result
    return jnp.clip(result, min=-limit, max=limit).astype(dtype)


def setup_inputs(seed: int = 0) -> dict:
    key_of = jax.random.split(jax.random.key(seed), 8)
    inputs = scatter_about(key_of[0], (SEQS, SEQ, D), 1.0, 6.0, ((0, 8), (1, 4)))
    queries = scatter_about(key_of[1], (SEQS, SEQ, WIDTH), 1.0, 6.0, ((0, 8), (1, 4)))
    keys = scatter_about(key_of[2], (SEQS, SEQ, WIDTH), 0.25, 1.5, ((0, 8), (1, 4)))
    values = scatter_about(key_of[3], (SEQS, SEQ, WIDTH), 1.0, 6.0, ((0, 8), (1, 4)))
    log_decay = draw_log_decay(jax.random.fold_in(key_of[7], 71), 0)
    cotangent = scatter_about(key_of[5], (SEQS, SEQ, WIDTH), 0.1, 0.59765625, ((0, 8), (1, 4)))
    value_weight = scatter_about(key_of[6], (D, WIDTH), D ** -0.5, 0.125, ((0, 8),))
    return {"inputs": inputs, "queries": queries, "keys": keys, "values": values, "log_decay": log_decay, "cotangent": cotangent, "value_weight": value_weight}


def combine(earlier, later):
    first_decay, first_state = earlier
    second_decay, second_state = later
    return (first_decay * second_decay, second_decay[..., None] * first_state + second_state)

def carry_scan(decays, updates):
    return lax.associative_scan(combine, (decays, updates), axis=0)[1]

def to_blocks(rows, num_blocks):
    length, groups, width = rows.shape
    return jnp.transpose(rows.astype(jnp.float32).reshape(num_blocks, BLOCK, groups, width), (0, 2, 3, 1))

def mixing(query_rows, key_rows, value_rows, gate_rows):
    length, groups, key_width = query_rows.shape
    value_width = value_rows.shape[2]
    num_blocks = length // BLOCK
    scaled_query = to_blocks(query_rows, num_blocks) * HEAD_DIM ** (-0.5)
    key_float = to_blocks(key_rows, num_blocks)
    value_float = to_blocks(value_rows, num_blocks)
    gate_float = to_blocks(gate_rows, num_blocks)
    running = jnp.cumsum(gate_float, axis=3)
    exclusive = running - gate_float
    block_end = running[..., -1]
    lower_mask = jnp.tril(jnp.ones((BLOCK, BLOCK), jnp.float32))
    upper_mask = lower_mask.T
    query_fwd = scaled_query * jnp.exp(running)
    key_fwd = key_float * jnp.exp(-running)
    scores_fwd = jnp.einsum('ngcr,ngcs->ngrs', query_fwd, key_fwd) * lower_mask
    key_end = key_float * jnp.exp(block_end[..., None] - running)
    states = carry_scan(jnp.exp(block_end), jnp.einsum('ngcs,ngvs->ngcv', key_end, value_float))
    before = jnp.concatenate([jnp.zeros_like(states[:1]), states[:-1]], axis=0)
    out_fwd = jnp.einsum('ngrs,ngvs->ngvr', scores_fwd, value_float) + jnp.einsum('ngcr,ngcv->ngvr', query_fwd, before)
    query_bwd = scaled_query * jnp.exp(-exclusive)
    key_bwd = key_float * jnp.exp(exclusive)
    scores_bwd = jnp.einsum('ngcr,ngcs->ngrs', query_bwd, key_bwd) * upper_mask
    rights = jnp.flip(carry_scan(jnp.flip(jnp.exp(block_end), 0), jnp.flip(jnp.einsum('ngcs,ngvs->ngcv', key_bwd, value_float), 0)), 0)
    after = jnp.concatenate([rights[1:], jnp.zeros_like(rights[:1])], axis=0)
    query_read = scaled_query * jnp.exp(block_end[..., None] - exclusive)
    out_bwd = jnp.einsum('ngrs,ngvs->ngvr', scores_bwd, value_float) + jnp.einsum('ngcr,ngcv->ngvr', query_read, after)
    total = out_fwd + out_bwd
    return jnp.transpose(total, (0, 3, 1, 2)).reshape(length, groups, value_width)

def reference(inputs, queries, keys, values, log_decay, cotangent, value_weight):
    seq_len = queries.shape[1]
    width = queries.shape[2]

    def per_group(array):
        spread = jnp.broadcast_to(array.reshape(seq_len, HEADS, 1, HEAD_DIM), (seq_len, HEADS, 2, HEAD_DIM))
        return spread.reshape(seq_len, GROUPS, HEAD_DIM)

    def one_sequence(pieces):
        query_seq, key_seq, value_seq, gate_seq, upstream = pieces
        _, pullback = jax.vjp(mixing, query_seq.reshape(seq_len, GROUPS, HALF), key_seq.reshape(seq_len, GROUPS, HALF), per_group(value_seq), gate_seq.reshape(seq_len, GROUPS, HALF))
        grad_q, grad_k, grad_v, grad_g = pullback(per_group(upstream).astype(jnp.float32))
        value_sum = lax.optimization_barrier(jnp.sum(grad_v.astype(jnp.bfloat16).astype(jnp.float32).reshape(seq_len, HEADS, 2, HEAD_DIM), axis=2))
        return (grad_q.astype(jnp.bfloat16).reshape(seq_len, width), grad_k.astype(jnp.bfloat16).reshape(seq_len, width), grad_g.astype(jnp.bfloat16).reshape(seq_len, width), value_sum.astype(jnp.bfloat16).reshape(seq_len, width))
    grad_queries, grad_keys, grad_decay, value_grad = lax.map(one_sequence, (queries, keys, values, log_decay, cotangent))
    flat_inputs = inputs.reshape(-1, inputs.shape[2])
    flat_grad = value_grad.reshape(-1, width)
    grad_inputs = jnp.dot(flat_grad, value_weight.T, preferred_element_type=jnp.float32).astype(jnp.bfloat16).reshape(inputs.shape)
    grad_weight = jnp.dot(flat_inputs.T, flat_grad, preferred_element_type=jnp.float32)
    return (grad_queries, grad_keys, grad_decay, grad_inputs, grad_weight)
```

```python
import functools

import jax
import jax.numpy as jnp
from jax import lax
from jax.experimental import pallas as pl
from jax.experimental.pallas import tpu as pltpu
from jax.sharding import PartitionSpec as P

HEAD_DIM = 64
PAIR = 2 * HEAD_DIM
SCALE = HEAD_DIM ** (-0.5)
BF = jnp.bfloat16
F32 = jnp.float32


def dot(a, b, ca, cb):
    return lax.dot_general(a, b, (((ca,), (cb,)), ((), ())), preferred_element_type=F32)


def iotas(rows, cols):
    return (
        lax.broadcasted_iota(jnp.int32, (rows, cols), 0),
        lax.broadcasted_iota(jnp.int32, (rows, cols), 1),
    )


def first_head(rows):
    return iotas(rows, PAIR)[1] < HEAD_DIM


def running_sums(gate):
    length = gate.shape[0]
    row, col = iotas(length, length)
    running = dot((row >= col).astype(BF), gate, 1, 0)
    return running, running - gate.astype(F32), running[length - 1 : length]


def pack(full):
    return jnp.where(first_head(HEAD_DIM), full[:HEAD_DIM], full[HEAD_DIM:])


def unpack(state):
    mine = first_head(HEAD_DIM)
    zero = jnp.zeros_like(state)
    return jnp.concatenate([jnp.where(mine, state, zero), jnp.where(mine, zero, state)], axis=0)


def both_heads(rows):
    mine = first_head(rows.shape[0])
    zero = jnp.zeros_like(rows)
    return jnp.where(mine, rows, zero), jnp.where(mine, zero, rows)


def lanes(pair):
    return slice(pair * PAIR, (pair + 1) * PAIR)


def state_rows(pair):
    return slice(pair * HEAD_DIM, (pair + 1) * HEAD_DIM)


def read_states_kernel(place, q_ref, g_ref, o_ref, *out, pairs, seq_devices):
    me = place[0]
    high, low = [], []
    for pair in range(pairs):
        at = lanes(pair)
        running, exclusive, total = running_sums(g_ref[:, at])
        query = q_ref[:, at].astype(F32) * SCALE
        both = jnp.concatenate(
            [
                (query * jnp.exp(running)).astype(BF),
                (query * jnp.exp(total - exclusive)).astype(BF),
            ],
            axis=1,
        )
        full = dot(o_ref[:, at], both, 0, 0)
        to_earlier = pack(full[:, :PAIR]).astype(BF)
        to_later = pack(full[:, PAIR:]).astype(BF)
        for shift in range(1, seq_devices):
            later = jnp.full((HEAD_DIM, PAIR), me + shift, jnp.int32) < seq_devices
            out[shift - 1][state_rows(pair), :] = jnp.where(
                later, to_later.astype(F32), to_earlier.astype(F32)
            ).astype(BF)
        decay = jnp.exp(total)
        top = decay.astype(BF).astype(F32)
        high.append(top)
        low.append(decay - top)
    decays = jnp.concatenate(high + low, axis=0).astype(BF)
    for shift in range(1, seq_devices):
        out[shift - 1][pairs * HEAD_DIM :, :] = decays


def inner_values_kernel(place, q_ref, k_ref, v_ref, g_ref, o_ref, *out, pairs, seq_devices):
    me = place[0]
    inner_ref = out[0]
    length = q_ref.shape[0]
    row, col = iotas(length, length)
    for pair in range(pairs):
        at = lanes(pair)
        running, exclusive, total = running_sums(g_ref[:, at])
        query = q_ref[:, at].astype(F32) * SCALE
        key = k_ref[:, at].astype(F32)
        query_fwd = (query * jnp.exp(running)).astype(BF)
        query_bwd = (query * jnp.exp(-exclusive)).astype(BF)
        key_fwd = both_heads((key * jnp.exp(-running)).astype(BF))
        key_late = (key * jnp.exp(exclusive)).astype(BF)
        key_bwd = both_heads(key_late)
        key_end = (key * jnp.exp(total - running)).astype(BF)
        scores = []
        for head in range(2):
            ahead = dot(key_fwd[head], query_fwd, 1, 1)
            behind = dot(key_bwd[head], query_bwd, 1, 1)
            scores.append(
                (jnp.where(row <= col, ahead, 0.0) + jnp.where(row >= col, behind, 0.0)).astype(BF)
            )
        upstream = o_ref[:, at]
        inner_ref[:, at] = dot(
            jnp.concatenate(scores, axis=1), jnp.concatenate(both_heads(upstream), axis=0), 1, 0
        )
        full = dot(v_ref[:, at], jnp.concatenate([key_end, key_late], axis=1), 0, 0)
        to_later = pack(full[:, :PAIR])
        to_earlier = pack(full[:, PAIR:])
        for shift in range(1, seq_devices):
            later = jnp.full((HEAD_DIM, PAIR), me + shift, jnp.int32) < seq_devices
            out[shift][state_rows(pair), :] = jnp.where(later, to_later, to_earlier).astype(BF)


def gather_states(me, messages, decays, pair, seq_devices):
    before = jnp.zeros((HEAD_DIM, PAIR), F32)
    after = jnp.zeros((HEAD_DIM, PAIR), F32)
    weight_before = jnp.ones((1, PAIR), F32)
    weight_after = jnp.ones((1, PAIR), F32)

    def state(shift):
        return messages[shift - 1][state_rows(pair), :].astype(F32)

    for shift in range(1, seq_devices):
        earlier = jnp.full((HEAD_DIM, PAIR), me, jnp.int32) >= shift
        before = before + jnp.where(earlier, weight_before * state(shift), 0.0)
        weight_before = weight_before * decays(shift)
    for shift in range(seq_devices - 1, 0, -1):
        later = jnp.full((HEAD_DIM, PAIR), me, jnp.int32) < shift
        after = after + jnp.where(later, weight_after * state(shift), 0.0)
        weight_after = weight_after * decays(shift)
    return before, after


def decay_reader(messages, pair, pairs):
    base = pairs * HEAD_DIM

    def decays(shift):
        tail = messages[shift - 1][base : base + 2 * pairs, :].astype(F32)
        return tail[pair : pair + 1] + tail[pairs + pair : pairs + pair + 1]

    return decays


def values_kernel(place, k_ref, g_ref, inner_ref, *rest, pairs, seq_devices):
    me = place[0]
    messages = rest[: seq_devices - 1]
    value_ref, before_ref, after_ref = rest[seq_devices - 1 :]
    width = value_ref.shape[2]
    for pair in range(pairs):
        at = lanes(pair)
        running, exclusive, total = running_sums(g_ref[:, at])
        key = k_ref[:, at].astype(F32)
        before, after = gather_states(
            me, messages, decay_reader(messages, pair, pairs), pair, seq_devices
        )
        before_ref[state_rows(pair), :] = before
        after_ref[state_rows(pair), :] = after
        keys = jnp.concatenate(
            [
                (key * jnp.exp(total - running)).astype(BF),
                (key * jnp.exp(exclusive)).astype(BF),
            ],
            axis=1,
        )
        states = jnp.concatenate([unpack(after), unpack(before)], axis=1).astype(BF)
        grad = (inner_ref[:, at] + dot(keys, states, 1, 1)).astype(BF)
        step = min(width, PAIR)
        for start in range(0, PAIR, step):
            block, offset = divmod(pair * PAIR + start, width)
            value_ref[block, :, offset : offset + step] = grad[:, start : start + step]


def rest_kernel(place, q_ref, k_ref, v_ref, g_ref, o_ref, before_ref, after_ref, *rest, pairs, seq_devices):
    me = place[0]
    count = seq_devices - 1
    read_messages = rest[:count]
    write_messages = rest[count : 2 * count]
    gq_ref, gk_ref, gg_ref = rest[2 * count :]
    length = q_ref.shape[0]
    row, col = iotas(length, length)
    tail = (row <= col).astype(BF)
    for pair in range(pairs):
        at = lanes(pair)
        running, exclusive, total = running_sums(g_ref[:, at])
        query = q_ref[:, at].astype(F32)
        key = k_ref[:, at].astype(F32)
        value = v_ref[:, at]
        upstream = o_ref[:, at]
        grow_run = jnp.exp(running)
        shrink_run = jnp.exp(-running)
        grow_exc = jnp.exp(exclusive)
        shrink_exc = jnp.exp(-exclusive)
        end = jnp.exp(total)
        query_fwd = query * (SCALE * grow_run)
        query_bwd = query * (SCALE * shrink_exc)
        key_fwd = key * shrink_run
        key_bwd = key * grow_exc
        read_before = before_ref[state_rows(pair), :]
        read_after = after_ref[state_rows(pair), :]
        before, after = gather_states(
            me, write_messages, decay_reader(read_messages, pair, pairs), pair, seq_devices
        )
        write_own = pack(dot(value, (key * jnp.exp(total - running)).astype(BF), 0, 0))
        read_own = pack(
            dot(upstream, (query * (SCALE * jnp.exp(total - exclusive))).astype(BF), 0, 0)
        )
        through = jnp.sum(
            (end * before + write_own) * read_after + (end * read_before + read_own) * after,
            axis=0,
            keepdims=True,
        )
        value_heads = both_heads(value)
        upstream_heads = both_heads(upstream)
        low, high, low_turned, high_turned = [], [], [], []
        for head in range(2):
            product = dot(upstream_heads[head], value, 1, 1)
            turned = dot(value_heads[head], upstream, 1, 1)
            low.append(jnp.where(row >= col, product, 0.0).astype(BF))
            high.append(jnp.where(row <= col, product, 0.0).astype(BF))
            low_turned.append(jnp.where(row <= col, turned, 0.0).astype(BF))
            high_turned.append(jnp.where(row >= col, turned, 0.0).astype(BF))

        def total_of(blocks, outer, rows, state):
            left = jnp.concatenate(blocks + [outer], axis=1)
            right = jnp.concatenate(both_heads(rows.astype(BF)) + (unpack(state).astype(BF),), axis=0)
            return dot(left, right, 1, 0)

        gq_fwd = total_of(low, upstream, key_fwd, before) * (SCALE * grow_run)
        gq_bwd = total_of(high, upstream, key_bwd, after * end) * (SCALE * shrink_exc)
        gk_fwd = total_of(low_turned, value, query_fwd, read_after * end) * shrink_run
        gk_bwd = total_of(high_turned, value, query_bwd, read_before) * grow_exc
        gq_ref[:, at] = (gq_fwd + gq_bwd).astype(BF)
        gk_ref[:, at] = (gk_fwd + gk_bwd).astype(BF)
        backward = key * gk_bwd - query * gq_bwd
        change = query * gq_fwd - key * gk_fwd + backward
        top = change.astype(BF)
        bottom = (change - top.astype(F32)).astype(BF)
        summed = dot(tail, jnp.concatenate([top, bottom], axis=1), 1, 0)
        gg_ref[:, at] = (summed[:, :PAIR] + summed[:, PAIR:] - backward + through).astype(BF)


def source_of(place, step, row_devices):
    chips = row_devices // 2
    mine = place[1]
    core = lax.rem(mine, 2)
    chip = lax.rem(lax.div(mine, 2) + chips - step // 2, chips)
    return 2 * chip + (core if step % 2 == 0 else 1 - core)


def weight_kernel(place, x_ref, *rest, row_devices):
    pieces = rest[:row_devices]
    out_ref = rest[row_devices]
    for block in range(out_ref.shape[0]):
        acc = jnp.zeros(out_ref.shape[1:], F32)
        for step in range(row_devices):
            acc = acc + dot(x_ref[source_of(place, step, row_devices)], pieces[step][block], 1, 0)
        out_ref[block] = acc.astype(BF)


def inputs_kernel(place, w_ref, *rest, row_devices):
    pieces = rest[:row_devices]
    out_ref = rest[row_devices]
    blocks, _, width = pieces[0].shape
    for step in range(row_devices):
        acc = jnp.zeros(out_ref.shape[1:], F32)
        for block in range(blocks):
            acc = acc + dot(pieces[step][block], w_ref[:, block * width : (block + 1) * width], 1, 1)
        out_ref[source_of(place, step, row_devices)] = acc.astype(BF)


def call(body, shapes, place, *operands, name):
    specs = [pl.BlockSpec(memory_space=pltpu.SMEM)] + [
        pl.BlockSpec(memory_space=pltpu.VMEM) for _ in operands
    ]
    return pl.pallas_call(
        body,
        out_shape=[jax.ShapeDtypeStruct(shape, dtype) for shape, dtype in shapes],
        in_specs=specs,
        out_specs=[pl.BlockSpec(memory_space=pltpu.VMEM) for _ in shapes],
        name=name,
    )(place, *operands)


def per_device(inputs, queries, keys, values, log_decay, cotangent, value_weight):
    seq_devices = lax.axis_size("sp")
    row_devices = lax.axis_size("dp")
    chips = row_devices // 2
    tokens, width = queries.shape[1:]
    pairs = width // PAIR
    rows = value_weight.shape[0]
    columns = width // seq_devices
    place = jnp.stack([lax.axis_index("sp"), lax.axis_index("dp")]).astype(jnp.int32)
    query, key, value, gate, upstream = (
        array[0] for array in (queries, keys, values, log_decay, cotangent)
    )
    sizes = dict(pairs=pairs, seq_devices=seq_devices)
    count = seq_devices - 1

    def around(messages):
        return [
            lax.ppermute(
                message, "sp", [(i, (i + shift) % seq_devices) for i in range(seq_devices)]
            )
            for shift, message in enumerate(messages, 1)
        ]

    read_own = call(
        functools.partial(read_states_kernel, **sizes),
        [((pairs * HEAD_DIM + 2 * pairs, PAIR), BF)] * count,
        place, query, gate, upstream, name="read_states",
    )
    read_other = around(read_own)
    inner, *write_own = call(
        functools.partial(inner_values_kernel, **sizes),
        [((tokens, width), F32)] + [((pairs * HEAD_DIM, PAIR), BF)] * count,
        place, query, key, value, gate, upstream, name="inner_values",
    )
    input_rows = lax.all_to_all(
        inputs[0].reshape(tokens, row_devices, rows).transpose(1, 2, 0), "dp", 0, 0, tiled=True
    )
    value_grad, before, after = call(
        functools.partial(values_kernel, **sizes),
        [((seq_devices, tokens, columns), BF)] + [((pairs * HEAD_DIM, PAIR), F32)] * 2,
        place, key, gate, inner, *read_other, name="value_grads",
    )
    write_own, value_grad = lax.optimization_barrier((write_own, value_grad))
    pieces = []
    for shift in range(chips):
        piece = value_grad
        if shift:
            piece = lax.ppermute(
                value_grad, "dp", [(i, (i + 2 * shift) % row_devices) for i in range(row_devices)]
            )
        swapped = lax.ppermute(piece, "dp", [(i, i ^ 1) for i in range(row_devices)])
        pieces += [piece, swapped]
    write_other = around(write_own)
    (partial,) = call(
        functools.partial(weight_kernel, row_devices=row_devices),
        [((seq_devices, rows, columns), BF)],
        place, input_rows, *pieces, name="weight_part",
    )
    shares = lax.all_to_all(partial, "sp", 0, 0, tiled=True)
    (token_rows,) = call(
        functools.partial(inputs_kernel, row_devices=row_devices),
        [((row_devices, tokens, rows), BF)],
        place, value_weight, *pieces, name="input_rows",
    )
    grad_inputs = (
        lax.all_to_all(token_rows, "dp", 0, 0, tiled=True)
        .transpose(1, 0, 2)
        .reshape(1, tokens, row_devices * rows)
    )
    grad_queries, grad_keys, grad_decay = call(
        functools.partial(rest_kernel, **sizes),
        [((tokens, width), BF)] * 3,
        place, query, key, value, gate, upstream, before, after, *read_other, *write_other,
        name="other_grads",
    )
    share = jnp.sum(shares.astype(F32), axis=0).astype(BF)
    grad_weight = lax.all_gather(share, "sp", axis=1, tiled=True).astype(F32)
    return (grad_queries[None], grad_keys[None], grad_decay[None], grad_inputs, grad_weight)


def solution(mesh):
    return jax.shard_map(
        per_device,
        mesh=mesh,
        in_specs=(P("dp", "sp", None),) * 6 + (P("dp", None),),
        out_specs=(P("dp", "sp", None),) * 4 + (P("dp", None),),
        check_vma=False,
    )
```

```python
import functools

import jax
import jax.numpy as jnp
from jax import lax
from jax.experimental import pallas as pl
from jax.experimental.pallas import tpu as pltpu
from jax.sharding import PartitionSpec as P

HEAD_DIM = 64
PAIR = 2 * HEAD_DIM
SCALE = HEAD_DIM ** (-0.5)
BF = jnp.bfloat16
F32 = jnp.float32


def dot(a, b, ca, cb):
    return lax.dot_general(a, b, (((ca,), (cb,)), ((), ())), preferred_element_type=F32)


def iotas(rows, cols):
    return (
        lax.broadcasted_iota(jnp.int32, (rows, cols), 0),
        lax.broadcasted_iota(jnp.int32, (rows, cols), 1),
    )


def first_head(rows):
    return iotas(rows, PAIR)[1] < HEAD_DIM


def running_sums(gate):
    length = gate.shape[0]
    row, col = iotas(length, length)
    running = dot((row >= col).astype(BF), gate, 1, 0)
    return running, running - gate.astype(F32), running[length - 1 : length]


def pack(full):
    return jnp.where(first_head(HEAD_DIM), full[:HEAD_DIM], full[HEAD_DIM:])


def unpack(state):
    mine = first_head(HEAD_DIM)
    zero = jnp.zeros_like(state)
    return jnp.concatenate([jnp.where(mine, state, zero), jnp.where(mine, zero, state)], axis=0)


def both_heads(rows):
    mine = first_head(rows.shape[0])
    zero = jnp.zeros_like(rows)
    return jnp.where(mine, rows, zero), jnp.where(mine, zero, rows)


def lanes(pair):
    return slice(pair * PAIR, (pair + 1) * PAIR)


def state_rows(pair):
    return slice(pair * HEAD_DIM, (pair + 1) * HEAD_DIM)


def read_states_kernel(place, q_ref, g_ref, o_ref, *out, pairs, seq_devices):
    me = place[0]
    high, low = [], []
    for pair in range(pairs):
        at = lanes(pair)
        running, exclusive, total = running_sums(g_ref[:, at])
        query = q_ref[:, at].astype(F32) * SCALE
        both = jnp.concatenate(
            [
                (query * jnp.exp(running)).astype(BF),
                (query * jnp.exp(total - exclusive)).astype(BF),
            ],
            axis=1,
        )
        full = dot(o_ref[:, at], both, 0, 0)
        to_earlier = pack(full[:, :PAIR]).astype(BF)
        to_later = pack(full[:, PAIR:]).astype(BF)
        for shift in range(1, seq_devices):
            later = jnp.full((HEAD_DIM, PAIR), me + shift, jnp.int32) < seq_devices
            out[shift - 1][state_rows(pair), :] = jnp.where(
                later, to_later.astype(F32), to_earlier.astype(F32)
            ).astype(BF)
        decay = jnp.exp(total)
        top = decay.astype(BF).astype(F32)
        high.append(top)
        low.append(decay - top)
    decays = jnp.concatenate(high + low, axis=0).astype(BF)
    for shift in range(1, seq_devices):
        out[shift - 1][pairs * HEAD_DIM :, :] = decays


def inner_values_kernel(place, q_ref, k_ref, v_ref, g_ref, o_ref, *out, pairs, seq_devices):
    me = place[0]
    inner_ref = out[0]
    length = q_ref.shape[0]
    row, col = iotas(length, length)
    for pair in range(pairs):
        at = lanes(pair)
        running, exclusive, total = running_sums(g_ref[:, at])
        query = q_ref[:, at].astype(F32) * SCALE
        key = k_ref[:, at].astype(F32)
        query_fwd = (query * jnp.exp(running)).astype(BF)
        query_bwd = (query * jnp.exp(-exclusive)).astype(BF)
        key_fwd = both_heads((key * jnp.exp(-running)).astype(BF))
        key_late = (key * jnp.exp(exclusive)).astype(BF)
        key_bwd = both_heads(key_late)
        key_end = (key * jnp.exp(total - running)).astype(BF)
        scores = []
        for head in range(2):
            ahead = dot(key_fwd[head], query_fwd, 1, 1)
            behind = dot(key_bwd[head], query_bwd, 1, 1)
            scores.append(
                (jnp.where(row <= col, ahead, 0.0) + jnp.where(row >= col, behind, 0.0)).astype(BF)
            )
        upstream = o_ref[:, at]
        inner_ref[:, at] = dot(
            jnp.concatenate(scores, axis=1), jnp.concatenate(both_heads(upstream), axis=0), 1, 0
        )
        full = dot(v_ref[:, at], jnp.concatenate([key_end, key_late], axis=1), 0, 0)
        to_later = pack(full[:, :PAIR])
        to_earlier = pack(full[:, PAIR:])
        for shift in range(1, seq_devices):
            later = jnp.full((HEAD_DIM, PAIR), me + shift, jnp.int32) < seq_devices
            out[shift][state_rows(pair), :] = jnp.where(later, to_later, to_earlier).astype(BF)


def gather_states(me, messages, decays, pair, seq_devices):
    before = jnp.zeros((HEAD_DIM, PAIR), F32)
    after = jnp.zeros((HEAD_DIM, PAIR), F32)
    weight_before = jnp.ones((1, PAIR), F32)
    weight_after = jnp.ones((1, PAIR), F32)

    def state(shift):
        return messages[shift - 1][state_rows(pair), :].astype(F32)

    for shift in range(1, seq_devices):
        earlier = jnp.full((HEAD_DIM, PAIR), me, jnp.int32) >= shift
        before = before + jnp.where(earlier, weight_before * state(shift), 0.0)
        weight_before = weight_before * decays(shift)
    for shift in range(seq_devices - 1, 0, -1):
        later = jnp.full((HEAD_DIM, PAIR), me, jnp.int32) < shift
        after = after + jnp.where(later, weight_after * state(shift), 0.0)
        weight_after = weight_after * decays(shift)
    return before, after


def decay_reader(messages, pair, pairs):
    base = pairs * HEAD_DIM

    def decays(shift):
        tail = messages[shift - 1][base : base + 2 * pairs, :].astype(F32)
        return tail[pair : pair + 1] + tail[pairs + pair : pairs + pair + 1]

    return decays


def values_kernel(place, k_ref, g_ref, inner_ref, *rest, pairs, seq_devices):
    me = place[0]
    count = seq_devices - 1
    messages = rest[:count]
    value_ref, before_ref, after_ref = rest[2 * count + 1 : 2 * count + 4]
    width = value_ref.shape[2]
    for pair in range(pairs):
        at = lanes(pair)
        running, exclusive, total = running_sums(g_ref[:, at])
        key = k_ref[:, at].astype(F32)
        before, after = gather_states(
            me, messages, decay_reader(messages, pair, pairs), pair, seq_devices
        )
        before_ref[state_rows(pair), :] = before
        after_ref[state_rows(pair), :] = after
        keys = jnp.concatenate(
            [
                (key * jnp.exp(total - running)).astype(BF),
                (key * jnp.exp(exclusive)).astype(BF),
            ],
            axis=1,
        )
        states = jnp.concatenate([unpack(after), unpack(before)], axis=1).astype(BF)
        grad = (inner_ref[:, at] + dot(keys, states, 1, 1)).astype(BF)
        step = min(width, PAIR)
        for start in range(0, PAIR, step):
            block, offset = divmod(pair * PAIR + start, width)
            value_ref[block, :, offset : offset + step] = grad[:, start : start + step]


def rest_kernel(place, q_ref, k_ref, v_ref, g_ref, o_ref, before_ref, after_ref, *rest, pairs, seq_devices):
    me = place[0]
    count = seq_devices - 1
    read_messages = rest[:count]
    write_messages = rest[count : 2 * count]
    gq_ref, gk_ref, gg_ref = rest[-3:]
    length = q_ref.shape[0]
    row, col = iotas(length, length)
    tail = (row <= col).astype(BF)
    for pair in range(pairs):
        at = lanes(pair)
        running, exclusive, total = running_sums(g_ref[:, at])
        query = q_ref[:, at].astype(F32)
        key = k_ref[:, at].astype(F32)
        value = v_ref[:, at]
        upstream = o_ref[:, at]
        grow_run = jnp.exp(running)
        shrink_run = jnp.exp(-running)
        grow_exc = jnp.exp(exclusive)
        shrink_exc = jnp.exp(-exclusive)
        end = jnp.exp(total)
        query_fwd = query * (SCALE * grow_run)
        query_bwd = query * (SCALE * shrink_exc)
        key_fwd = key * shrink_run
        key_bwd = key * grow_exc
        read_before = before_ref[state_rows(pair), :]
        read_after = after_ref[state_rows(pair), :]
        before, after = gather_states(
            me, write_messages, decay_reader(read_messages, pair, pairs), pair, seq_devices
        )
        write_own = pack(dot(value, (key * jnp.exp(total - running)).astype(BF), 0, 0))
        read_own = pack(
            dot(upstream, (query * (SCALE * jnp.exp(total - exclusive))).astype(BF), 0, 0)
        )
        through = jnp.sum(
            (end * before + write_own) * read_after + (end * read_before + read_own) * after,
            axis=0,
            keepdims=True,
        )
        value_heads = both_heads(value)
        upstream_heads = both_heads(upstream)
        low, high, low_turned, high_turned = [], [], [], []
        for head in range(2):
            product = dot(upstream_heads[head], value, 1, 1)
            turned = dot(value_heads[head], upstream, 1, 1)
            low.append(jnp.where(row >= col, product, 0.0).astype(BF))
            high.append(jnp.where(row <= col, product, 0.0).astype(BF))
            low_turned.append(jnp.where(row <= col, turned, 0.0).astype(BF))
            high_turned.append(jnp.where(row >= col, turned, 0.0).astype(BF))

        def total_of(blocks, outer, rows, state):
            left = jnp.concatenate(blocks + [outer], axis=1)
            right = jnp.concatenate(both_heads(rows.astype(BF)) + (unpack(state).astype(BF),), axis=0)
            return dot(left, right, 1, 0)

        gq_fwd = total_of(low, upstream, key_fwd, before) * (SCALE * grow_run)
        gq_bwd = total_of(high, upstream, key_bwd, after * end) * (SCALE * shrink_exc)
        gk_fwd = total_of(low_turned, value, query_fwd, read_after * end) * shrink_run
        gk_bwd = total_of(high_turned, value, query_bwd, read_before) * grow_exc
        gq_ref[:, at] = (gq_fwd + gq_bwd).astype(BF)
        gk_ref[:, at] = (gk_fwd + gk_bwd).astype(BF)
        backward = key * gk_bwd - query * gq_bwd
        change = query * gq_fwd - key * gk_fwd + backward
        top = change.astype(BF)
        bottom = (change - top.astype(F32)).astype(BF)
        summed = dot(tail, jnp.concatenate([top, bottom], axis=1), 1, 0)
        gg_ref[:, at] = (summed[:, :PAIR] + summed[:, PAIR:] - backward + through).astype(BF)


def source_of(place, step, row_devices):
    chips = row_devices // 2
    mine = place[1]
    core = lax.rem(mine, 2)
    chip = lax.rem(lax.div(mine, 2) + chips - step // 2, chips)
    return 2 * chip + (core if step % 2 == 0 else 1 - core)


def weight_kernel(place, x_ref, *rest, row_devices, seq_devices):
    pieces = rest[:row_devices]
    outs = rest[-seq_devices:]
    for shift, out_ref in enumerate(outs):
        block = lax.rem(place[0] + shift, seq_devices)
        acc = jnp.zeros(out_ref.shape, F32)
        for step in range(row_devices):
            acc = acc + dot(x_ref[source_of(place, step, row_devices)], pieces[step][block], 1, 0)
        out_ref[...] = acc.astype(out_ref.dtype)


def inputs_kernel(place, w_ref, *rest, row_devices):
    pieces = rest[:row_devices]
    out_ref = rest[-1]
    blocks, _, width = pieces[0].shape
    for step in range(row_devices):
        acc = jnp.zeros(out_ref.shape[1:], F32)
        for block in range(blocks):
            acc = acc + dot(pieces[step][block], w_ref[:, block * width : (block + 1) * width], 1, 1)
        out_ref[source_of(place, step, row_devices)] = acc.astype(BF)


def join_kernel(place, *rest, seq_devices):
    out_ref = rest[-1]
    width = rest[0].shape[1]
    for shift in range(seq_devices):
        source = lax.rem(place[0] + seq_devices - shift, seq_devices)
        for block in range(seq_devices):

            @pl.when(source == block)
            def _(shift=shift, block=block):
                out_ref[:, block * width : (block + 1) * width] = rest[shift][...].astype(F32)


def call(body, shapes, place, *operands, name, waits=(), through=()):
    vmem = pl.BlockSpec(memory_space=pltpu.VMEM)
    anywhere = pl.BlockSpec(memory_space=pl.ANY)
    first = 1 + len(operands) + len(waits)
    return pl.pallas_call(
        body,
        out_shape=[jax.ShapeDtypeStruct(shape, dtype) for shape, dtype in shapes]
        + [jax.ShapeDtypeStruct(array.shape, array.dtype) for array in through],
        in_specs=[pl.BlockSpec(memory_space=pltpu.SMEM)]
        + [vmem] * len(operands)
        + [anywhere] * (len(waits) + len(through)),
        out_specs=[vmem] * len(shapes) + [anywhere] * len(through),
        input_output_aliases={first + i: len(shapes) + i for i in range(len(through))},
        name=name,
    )(place, *operands, *waits, *through)


def per_device(inputs, queries, keys, values, log_decay, cotangent, value_weight):
    seq_devices = lax.axis_size("sp")
    row_devices = lax.axis_size("dp")
    chips = row_devices // 2
    tokens, width = queries.shape[1:]
    pairs = width // PAIR
    rows = value_weight.shape[0]
    columns = width // seq_devices
    place = jnp.stack([lax.axis_index("sp"), lax.axis_index("dp")]).astype(jnp.int32)
    query, key, value, gate, upstream = (
        array[0] for array in (queries, keys, values, log_decay, cotangent)
    )
    sizes = dict(pairs=pairs, seq_devices=seq_devices)
    count = seq_devices - 1

    def around(messages):
        return [
            lax.ppermute(
                message, "sp", [(i, (i + shift) % seq_devices) for i in range(seq_devices)]
            )
            for shift, message in enumerate(messages, 1)
        ]

    read_own = call(
        functools.partial(read_states_kernel, **sizes),
        [((pairs * HEAD_DIM + 2 * pairs, PAIR), BF)] * count,
        place, query, gate, upstream, name="read_states",
    )
    read_other = around(read_own)
    inner, *write_own = call(
        functools.partial(inner_values_kernel, **sizes),
        [((tokens, width), F32)] + [((pairs * HEAD_DIM, PAIR), BF)] * count,
        place, query, key, value, gate, upstream, name="inner_values",
    )
    input_rows = lax.all_to_all(
        inputs[0].reshape(tokens, row_devices, rows).transpose(1, 2, 0), "dp", 0, 0, tiled=True
    )
    value_grad, before, after, *write_own = call(
        functools.partial(values_kernel, **sizes),
        [((seq_devices, tokens, columns), BF)] + [((pairs * HEAD_DIM, PAIR), F32)] * 2,
        place, key, gate, inner, *read_other, name="value_grads",
        waits=(input_rows,), through=write_own,
    )
    pieces = []
    for shift in range(chips):
        piece = value_grad
        if shift:
            piece = lax.ppermute(
                value_grad, "dp", [(i, (i + 2 * shift) % row_devices) for i in range(row_devices)]
            )
        swapped = lax.ppermute(piece, "dp", [(i, i ^ 1) for i in range(row_devices)])
        pieces += [piece, swapped]
    write_other = around(write_own)
    partial = call(
        functools.partial(weight_kernel, row_devices=row_devices, seq_devices=seq_devices),
        [((rows, columns), F32)] + [((rows, columns), BF)] * count,
        place, input_rows, *pieces, name="weight_part", waits=write_other,
    )
    shares = around(partial[1:])
    (token_rows,) = call(
        functools.partial(inputs_kernel, row_devices=row_devices),
        [((row_devices, tokens, rows), BF)],
        place, value_weight, *pieces, name="input_rows", waits=partial[:1],
    )
    grad_inputs = (
        lax.all_to_all(token_rows, "dp", 0, 0, tiled=True)
        .transpose(1, 0, 2)
        .reshape(1, tokens, row_devices * rows)
    )
    grad_queries, grad_keys, grad_decay = call(
        functools.partial(rest_kernel, **sizes),
        [((tokens, width), BF)] * 3,
        place, query, key, value, gate, upstream, before, after, *read_other, *write_other,
        name="other_grads", waits=(token_rows,),
    )
    share = (partial[0] + sum(part.astype(F32) for part in shares)).astype(BF)
    (grad_weight,) = call(
        functools.partial(join_kernel, seq_devices=seq_devices),
        [((rows, width), F32)],
        place, share, *around([share] * count), name="join",
    )
    return (grad_queries[None], grad_keys[None], grad_decay[None], grad_inputs, grad_weight)


def solution(mesh):
    return jax.shard_map(
        per_device,
        mesh=mesh,
        in_specs=(P("dp", "sp", None),) * 6 + (P("dp", None),),
        out_specs=(P("dp", "sp", None),) * 4 + (P("dp", None),),
        check_vma=False,
    )
```

```python
import functools

import jax
import jax.numpy as jnp
from jax import lax
from jax.experimental import pallas as pl
from jax.experimental.pallas import tpu as pltpu
from jax.sharding import PartitionSpec as P


HEAD_DIM = 64
PAIR = 2 * HEAD_DIM
SCALE = HEAD_DIM ** (-0.5)
BF = jnp.bfloat16
F32 = jnp.float32


def dot(a, b, ca, cb):
    return lax.dot_general(a, b, (((ca,), (cb,)), ((), ())), preferred_element_type=F32)


def iotas(rows, cols):
    return (
        lax.broadcasted_iota(jnp.int32, (rows, cols), 0),
        lax.broadcasted_iota(jnp.int32, (rows, cols), 1),
    )


def first_head(rows):
    return iotas(rows, PAIR)[1] < HEAD_DIM


def running_sums(gate):
    length = gate.shape[0]
    row, col = iotas(length, length)
    running = dot((row >= col).astype(BF), gate, 1, 0)
    return running, running - gate.astype(F32), running[length - 1 : length]


def pack(full):
    return jnp.where(first_head(HEAD_DIM), full[:HEAD_DIM], full[HEAD_DIM:])


def unpack(state):
    mine = first_head(HEAD_DIM)
    zero = jnp.zeros_like(state)
    return jnp.concatenate([jnp.where(mine, state, zero), jnp.where(mine, zero, state)], axis=0)


def both_heads(rows):
    mine = first_head(rows.shape[0])
    zero = jnp.zeros_like(rows)
    return jnp.where(mine, rows, zero), jnp.where(mine, zero, rows)


def lanes(pair):
    return slice(pair * PAIR, (pair + 1) * PAIR)


def state_rows(pair):
    return slice(pair * HEAD_DIM, (pair + 1) * HEAD_DIM)


def read_states_kernel(place, q_ref, g_ref, o_ref, *out, pairs, seq_devices):
    me = place[0]
    high, low = [], []
    for pair in range(pairs):
        at = lanes(pair)
        running, exclusive, total = running_sums(g_ref[:, at])
        query = q_ref[:, at].astype(F32) * SCALE
        both = jnp.concatenate(
            [
                (query * jnp.exp(running)).astype(BF),
                (query * jnp.exp(total - exclusive)).astype(BF),
            ],
            axis=1,
        )
        full = dot(o_ref[:, at], both, 0, 0)
        to_earlier = pack(full[:, :PAIR]).astype(BF)
        to_later = pack(full[:, PAIR:]).astype(BF)
        for shift in range(1, seq_devices):
            later = jnp.full((HEAD_DIM, PAIR), me + shift, jnp.int32) < seq_devices
            out[shift - 1][state_rows(pair), :] = jnp.where(
                later, to_later.astype(F32), to_earlier.astype(F32)
            ).astype(BF)
        decay = jnp.exp(total)
        top = decay.astype(BF).astype(F32)
        high.append(top)
        low.append(decay - top)
    decays = jnp.concatenate(high + low, axis=0).astype(BF)
    for shift in range(1, seq_devices):
        out[shift - 1][pairs * HEAD_DIM :, :] = decays


def inner_values_kernel(place, q_ref, k_ref, v_ref, g_ref, o_ref, *out, pairs, seq_devices):
    me = place[0]
    inner_ref = out[0]
    length = q_ref.shape[0]
    row, col = iotas(length, length)
    for pair in range(pairs):
        at = lanes(pair)
        running, exclusive, total = running_sums(g_ref[:, at])
        query = q_ref[:, at].astype(F32) * SCALE
        key = k_ref[:, at].astype(F32)
        query_fwd = (query * jnp.exp(running)).astype(BF)
        query_bwd = (query * jnp.exp(-exclusive)).astype(BF)
        key_fwd = both_heads((key * jnp.exp(-running)).astype(BF))
        key_late = (key * jnp.exp(exclusive)).astype(BF)
        key_bwd = both_heads(key_late)
        key_end = (key * jnp.exp(total - running)).astype(BF)
        scores = []
        for head in range(2):
            ahead = dot(key_fwd[head], query_fwd, 1, 1)
            behind = dot(key_bwd[head], query_bwd, 1, 1)
            scores.append(
                (jnp.where(row <= col, ahead, 0.0) + jnp.where(row >= col, behind, 0.0)).astype(BF)
            )
        upstream = o_ref[:, at]
        inner_ref[:, at] = dot(
            jnp.concatenate(scores, axis=1), jnp.concatenate(both_heads(upstream), axis=0), 1, 0
        )
        full = dot(v_ref[:, at], jnp.concatenate([key_end, key_late], axis=1), 0, 0)
        to_later = pack(full[:, :PAIR])
        to_earlier = pack(full[:, PAIR:])
        for shift in range(1, seq_devices):
            later = jnp.full((HEAD_DIM, PAIR), me + shift, jnp.int32) < seq_devices
            out[shift][state_rows(pair), :] = jnp.where(later, to_later, to_earlier).astype(BF)


def gather_states(me, messages, decays, pair, seq_devices):
    before = jnp.zeros((HEAD_DIM, PAIR), F32)
    after = jnp.zeros((HEAD_DIM, PAIR), F32)
    weight_before = jnp.ones((1, PAIR), F32)
    weight_after = jnp.ones((1, PAIR), F32)

    def state(shift):
        return messages[shift - 1][state_rows(pair), :].astype(F32)

    for shift in range(1, seq_devices):
        earlier = jnp.full((HEAD_DIM, PAIR), me, jnp.int32) >= shift
        before = before + jnp.where(earlier, weight_before * state(shift), 0.0)
        weight_before = weight_before * decays(shift)
    for shift in range(seq_devices - 1, 0, -1):
        later = jnp.full((HEAD_DIM, PAIR), me, jnp.int32) < shift
        after = after + jnp.where(later, weight_after * state(shift), 0.0)
        weight_after = weight_after * decays(shift)
    return before, after


def decay_reader(messages, pair, pairs):
    base = pairs * HEAD_DIM

    def decays(shift):
        tail = messages[shift - 1][base : base + 2 * pairs, :].astype(F32)
        return tail[pair : pair + 1] + tail[pairs + pair : pairs + pair + 1]

    return decays


def values_kernel(place, k_ref, g_ref, inner_ref, *rest, pairs, seq_devices):
    me = place[0]
    count = seq_devices - 1
    messages = rest[:count]
    value_ref, before_ref, after_ref = rest[2 * count : 2 * count + 3]
    width = value_ref.shape[2]
    for pair in range(pairs):
        at = lanes(pair)
        running, exclusive, total = running_sums(g_ref[:, at])
        key = k_ref[:, at].astype(F32)
        before, after = gather_states(
            me, messages, decay_reader(messages, pair, pairs), pair, seq_devices
        )
        before_ref[state_rows(pair), :] = before
        after_ref[state_rows(pair), :] = after
        keys = jnp.concatenate(
            [
                (key * jnp.exp(total - running)).astype(BF),
                (key * jnp.exp(exclusive)).astype(BF),
            ],
            axis=1,
        )
        states = jnp.concatenate([unpack(after), unpack(before)], axis=1).astype(BF)
        grad = (inner_ref[:, at] + dot(keys, states, 1, 1)).astype(BF)
        step = min(width, PAIR)
        for start in range(0, PAIR, step):
            block, offset = divmod(pair * PAIR + start, width)
            value_ref[block, :, offset : offset + step] = grad[:, start : start + step]


def rest_kernel(place, q_ref, k_ref, v_ref, g_ref, o_ref, before_ref, after_ref, *rest, pairs, seq_devices):
    me = place[0]
    count = seq_devices - 1
    read_messages = rest[:count]
    write_messages = rest[count : 2 * count]
    gq_ref, gk_ref, gg_ref = rest[-3:]
    length = q_ref.shape[0]
    row, col = iotas(length, length)
    tail = (row <= col).astype(BF)
    for pair in range(pairs):
        at = lanes(pair)
        running, exclusive, total = running_sums(g_ref[:, at])
        query = q_ref[:, at].astype(F32)
        key = k_ref[:, at].astype(F32)
        value = v_ref[:, at]
        upstream = o_ref[:, at]
        grow_run = jnp.exp(running)
        shrink_run = jnp.exp(-running)
        grow_exc = jnp.exp(exclusive)
        shrink_exc = jnp.exp(-exclusive)
        end = jnp.exp(total)
        query_fwd = query * (SCALE * grow_run)
        query_bwd = query * (SCALE * shrink_exc)
        key_fwd = key * shrink_run
        key_bwd = key * grow_exc
        read_before = before_ref[state_rows(pair), :]
        read_after = after_ref[state_rows(pair), :]
        before, after = gather_states(
            me, write_messages, decay_reader(read_messages, pair, pairs), pair, seq_devices
        )
        write_own = pack(dot(value, (key * jnp.exp(total - running)).astype(BF), 0, 0))
        read_own = pack(
            dot(upstream, (query * (SCALE * jnp.exp(total - exclusive))).astype(BF), 0, 0)
        )
        through = jnp.sum(
            (end * before + write_own) * read_after + (end * read_before + read_own) * after,
            axis=0,
            keepdims=True,
        )
        value_heads = both_heads(value)
        upstream_heads = both_heads(upstream)
        low, high, low_turned, high_turned = [], [], [], []
        for head in range(2):
            product = dot(upstream_heads[head], value, 1, 1)
            turned = dot(value_heads[head], upstream, 1, 1)
            low.append(jnp.where(row >= col, product, 0.0).astype(BF))
            high.append(jnp.where(row <= col, product, 0.0).astype(BF))
            low_turned.append(jnp.where(row <= col, turned, 0.0).astype(BF))
            high_turned.append(jnp.where(row >= col, turned, 0.0).astype(BF))

        def total_of(blocks, outer, rows, state):
            left = jnp.concatenate(blocks + [outer], axis=1)
            right = jnp.concatenate(both_heads(rows.astype(BF)) + (unpack(state).astype(BF),), axis=0)
            return dot(left, right, 1, 0)

        gq_fwd = total_of(low, upstream, key_fwd, before) * (SCALE * grow_run)
        gq_bwd = total_of(high, upstream, key_bwd, after * end) * (SCALE * shrink_exc)
        gk_fwd = total_of(low_turned, value, query_fwd, read_after * end) * shrink_run
        gk_bwd = total_of(high_turned, value, query_bwd, read_before) * grow_exc
        gq_ref[:, at] = (gq_fwd + gq_bwd).astype(BF)
        gk_ref[:, at] = (gk_fwd + gk_bwd).astype(BF)
        backward = key * gk_bwd - query * gq_bwd
        change = query * gq_fwd - key * gk_fwd + backward
        top = change.astype(BF)
        bottom = (change - top.astype(F32)).astype(BF)
        summed = dot(tail, jnp.concatenate([top, bottom], axis=1), 1, 0)
        gg_ref[:, at] = (summed[:, :PAIR] + summed[:, PAIR:] - backward + through).astype(BF)


def source_of(place, step, row_devices):
    chips = row_devices // 2
    mine = place[1]
    core = lax.rem(mine, 2)
    chip = lax.rem(lax.div(mine, 2) + chips - step // 2, chips)
    return 2 * chip + (core if step % 2 == 0 else 1 - core)


def weight_kernel(place, x_ref, *rest, row_devices, seq_devices):
    pieces = rest[:row_devices]
    outs = rest[-seq_devices:]
    for shift, out_ref in enumerate(outs):
        block = lax.rem(place[0] + shift, seq_devices)
        acc = jnp.zeros(out_ref.shape, F32)
        for step in range(row_devices):
            acc = acc + dot(x_ref[source_of(place, step, row_devices)], pieces[step][block], 1, 0)
        out_ref[...] = acc.astype(out_ref.dtype)


def inputs_kernel(place, w_ref, *rest, row_devices):
    pieces = rest[:row_devices]
    out_ref = rest[-1]
    blocks, _, width = pieces[0].shape
    for step in range(row_devices):
        acc = jnp.zeros(out_ref.shape[1:], F32)
        for block in range(blocks):
            acc = acc + dot(pieces[step][block], w_ref[:, block * width : (block + 1) * width], 1, 1)
        out_ref[source_of(place, step, row_devices)] = acc.astype(BF)


def join_kernel(place, *rest, seq_devices):
    out_ref = rest[-1]
    width = rest[0].shape[1]
    for shift in range(seq_devices):
        source = lax.rem(place[0] + seq_devices - shift, seq_devices)
        for block in range(seq_devices):

            @pl.when(source == block)
            def _(shift=shift, block=block):
                out_ref[:, block * width : (block + 1) * width] = rest[shift][...].astype(F32)


def call(body, shapes, place, *operands, waits=(), through=()):
    vmem = pl.BlockSpec(memory_space=pltpu.VMEM)
    anywhere = pl.BlockSpec(memory_space=pl.ANY)
    first = 1 + len(operands) + len(waits)
    return pl.pallas_call(
        body,
        out_shape=[jax.ShapeDtypeStruct(shape, dtype) for shape, dtype in shapes]
        + [jax.ShapeDtypeStruct(array.shape, array.dtype) for array in through],
        in_specs=[pl.BlockSpec(memory_space=pltpu.SMEM)]
        + [vmem] * len(operands)
        + [anywhere] * (len(waits) + len(through)),
        out_specs=[vmem] * len(shapes) + [anywhere] * len(through),
        input_output_aliases={first + i: len(shapes) + i for i in range(len(through))},
    )(place, *operands, *waits, *through)


def per_device(inputs, queries, keys, values, log_decay, cotangent, value_weight):
    seq_devices = lax.axis_size("sp")
    row_devices = lax.axis_size("dp")
    chips = row_devices // 2
    tokens, width = queries.shape[1:]
    pairs = width // PAIR
    rows = value_weight.shape[0]
    columns = width // seq_devices
    place = jnp.stack([lax.axis_index("sp"), lax.axis_index("dp")]).astype(jnp.int32)
    query, key, value, gate, upstream = (
        array[0] for array in (queries, keys, values, log_decay, cotangent)
    )
    sizes = dict(pairs=pairs, seq_devices=seq_devices)
    count = seq_devices - 1

    def around(messages):
        return [
            lax.ppermute(
                message, "sp", [(i, (i + shift) % seq_devices) for i in range(seq_devices)]
            )
            for shift, message in enumerate(messages, 1)
        ]

    read_own = call(
        functools.partial(read_states_kernel, **sizes),
        [((pairs * HEAD_DIM + 2 * pairs, PAIR), BF)] * count,
        place, query, gate, upstream,
    )
    read_other = around(read_own)
    inner, *write_own = call(
        functools.partial(inner_values_kernel, **sizes),
        [((tokens, width), F32)] + [((pairs * HEAD_DIM, PAIR), BF)] * count,
        place, query, key, value, gate, upstream,
    )
    input_rows = lax.all_to_all(
        inputs[0].reshape(tokens, row_devices, rows).transpose(1, 2, 0), "dp", 0, 0, tiled=True
    )
    value_grad, before, after, *write_own = call(
        functools.partial(values_kernel, **sizes),
        [((seq_devices, tokens, columns), BF)] + [((pairs * HEAD_DIM, PAIR), F32)] * 2,
        place, key, gate, inner, *read_other,
        through=write_own,
    )
    write_other = around(write_own)
    pieces = []
    for shift in range(chips):
        piece = value_grad
        if shift:
            piece = lax.ppermute(
                value_grad, "dp", [(i, (i + 2 * shift) % row_devices) for i in range(row_devices)]
            )
        swapped = lax.ppermute(piece, "dp", [(i, i ^ 1) for i in range(row_devices)])
        pieces += [piece, swapped]
    partial = call(
        functools.partial(weight_kernel, row_devices=row_devices, seq_devices=seq_devices),
        [((rows, columns), F32)] + [((rows, columns), BF)] * count,
        place, input_rows, *pieces, waits=write_other,
    )
    shares = around(partial[1:])
    (token_rows,) = call(
        functools.partial(inputs_kernel, row_devices=row_devices),
        [((row_devices, tokens, rows), BF)],
        place, value_weight, *pieces, waits=partial[:1],
    )
    grad_inputs = (
        lax.all_to_all(token_rows, "dp", 0, 0, tiled=True)
        .transpose(1, 0, 2)
        .reshape(1, tokens, row_devices * rows)
    )
    grad_queries, grad_keys, grad_decay = call(
        functools.partial(rest_kernel, **sizes),
        [((tokens, width), BF)] * 3,
        place, query, key, value, gate, upstream, before, after, *read_other, *write_other,
        waits=(token_rows,),
    )
    share = (partial[0] + sum(part.astype(F32) for part in shares)).astype(BF)
    (grad_weight,) = call(
        functools.partial(join_kernel, seq_devices=seq_devices),
        [((rows, width), F32)],
        place, share, *around([share] * count),
        waits=(grad_inputs,),
    )
    return (grad_queries[None], grad_keys[None], grad_decay[None], grad_inputs, grad_weight)


def solution(mesh):
    return jax.shard_map(
        per_device,
        mesh=mesh,
        in_specs=(P("dp", "sp", None),) * 6 + (P("dp", None),),
        out_specs=(P("dp", "sp", None),) * 4 + (P("dp", None),),
        check_vma=False,
    )
```
